32 devices in a mesh: sp: 8 (over z, y), tp: 4 (over x, core).
Axes of the slice: x: 2, y: 2, z: 4, core: 2. Of those that a mesh axis runs over, the one named last changes fastest.
Arguments:
- residual: bfloat16 [3072, 2048], P('sp'), may hold values from -50 to 50
- queries_a: bfloat16 [3072, 512], P('sp', 'tp'), may hold values from -50 to 50
- keys_a: bfloat16 [3072, 512], P('sp', 'tp'), may hold values from -9 to 9
- values_a: bfloat16 [3072, 512], P('sp', 'tp'), may hold values from -6 to 6
- queries_b: bfloat16 [3072, 1024], P('sp', 'tp'), may hold values from -50 to 50
- keys_b: bfloat16 [3072, 1024], P('sp', 'tp'), may hold values from -9 to 9
- values_b: bfloat16 [3072, 512], P('sp', 'tp'), may hold values from -6 to 6
- mix_lambda: float32 [2, 4], P(None, 'tp'), may hold values from 0.3 to 0.8
- head_gain: float32 [2, 128], replicated, may hold values from 0.1 to 1.9
- out_a: bfloat16 [512, 2048], P('tp'), may hold values from -0.1875 to 0.1875
- out_b: bfloat16 [512, 2048], P('tp'), may hold values from -0.1875 to 0.1875
- norm_gain: float32 [2048], replicated, may hold values from 0.1 to 1.9
- w_gate: bfloat16 [2048, 5632], P('sp', 'tp'), may hold values from -0.125 to 0.125
- w_up: bfloat16 [2048, 5632], P('sp', 'tp'), may hold values from -0.125 to 0.125
- w_down: bfloat16 [5632, 2048], P('tp', 'sp'), may hold values from -0.21875 to 0.21875
Outputs:
- layer_out: bfloat16 [3072, 2048], P('sp', 'tp')
The draws below stay inside these ranges and needn't reach their ends.
All inputs are finite; a program needn't handle non-finite values.
Results may differ from the reference program's by a relative error of at most 0.0085.
Values may be sent and summed in bfloat16 or wider, within the bound.
A program may use at most 256 MiB of HBM per device.

```python
import math
import jax
import jax.numpy as jnp
from jax import lax

D = 2048
FF = 5632
HEADS = 4
QA = 64
QB = 128
VD = 128
TOKENS = 3072


def draw_residual(key, part):
    base = jax.random.fold_in(key, 3)
    first, second = jax.random.split(base, 2)
    column = jnp.arange(D, dtype=jnp.float32) / D
    noise = jnp.clip(jax.random.normal(first, (TOKENS, D), jnp.float32), -6.0, 6.0)
    columns = 0.4 * 10.0 ** column
    row_scale = 2.0 ** jax.random.uniform(second, (TOKENS, 1), jnp.float32, -1.0, 1.0)
    return (noise * columns[None, :] * row_scale).astype(jnp.bfloat16)


def paired(key, width, salt):
    base = jax.random.fold_in(key, salt)
    query_seed, key_seed = jax.random.split(base, 2)
    columns = HEADS * 2 * width
    queries = 1.3 * jnp.clip(jax.random.normal(query_seed, (TOKENS, columns), jnp.float32), -6.0, 6.0)
    keys = 1.3 * jnp.clip(jax.random.normal(key_seed, (TOKENS, columns), jnp.float32), -6.0, 6.0)
    return (queries, keys)


def draw_queries_a(key, part):
    return paired(key, QA, 11)[0].astype(jnp.bfloat16)


def draw_keys_a(key, part):
    return paired(key, QA, 11)[1].astype(jnp.bfloat16)


def draw_queries_b(key, part):
    return paired(key, QB, 13)[0].astype(jnp.bfloat16)


def draw_keys_b(key, part):
    return paired(key, QB, 13)[1].astype(jnp.bfloat16)


def block_scale(rng, extent, pieces, least, largest):
    def one(position, blocks):
        draws = jax.random.uniform(jax.random.fold_in(jax.random.fold_in(rng, 6), position), (blocks,), jnp.float32, least / len(pieces), largest / len(pieces))
        return jnp.repeat(jnp.exp(draws), extent[position] // blocks).reshape((-1,) + (1,) * (len(extent) - position - 1))

    level = one(*pieces[0])
    for cut in pieces[1:]:
        level = level * one(*cut)
    return level


def scatter_about(key, shape, scale, limit, cuts=(), kind=jnp.bfloat16):
    level = block_scale(key, shape, cuts, -0.22, 0.18) if cuts else 1.0
    values = jax.random.normal(key, shape, jnp.float32) * scale * level
    return jnp.minimum(jnp.maximum(values, -limit), limit).astype(kind)


def setup_inputs(seed: int = 0) -> dict:
    streams_of = jax.random.split(jax.random.key(seed), 16)
    return {
        "residual": draw_residual(jax.random.fold_in(streams_of[15], 71), 0),
        "queries_a": draw_queries_a(jax.random.fold_in(streams_of[15], 71), 0),
        "keys_a": draw_keys_a(jax.random.fold_in(streams_of[15], 71), 0),
        "values_a": scatter_about(streams_of[3], (TOKENS, HEADS * VD), 1.0, 6.0, ((0, 8), (1, 4))),
        "queries_b": draw_queries_b(jax.random.fold_in(streams_of[15], 71), 0),
        "keys_b": draw_keys_b(jax.random.fold_in(streams_of[15], 71), 0),
        "values_b": scatter_about(streams_of[6], (TOKENS, HEADS * VD), 1.0, 6.0, ((0, 8), (1, 4))),
        "mix_lambda": jnp.clip(0.3 + 0.5 * jax.random.uniform(streams_of[7], (2, HEADS), jnp.float32) ** block_scale(streams_of[7], (2, HEADS), ((1, 4),), -0.2, 0.2), 0.3, 0.8),
        "head_gain": jnp.clip(1.0 + 0.18 * jax.random.normal(streams_of[8], (2, VD), jnp.float32), 0.1, 1.9),
        "out_a": scatter_about(streams_of[9], (HEADS * VD, D), (2 * HEADS * VD) ** -0.5, 0.1875, ((0, 4),)),
        "out_b": scatter_about(streams_of[10], (HEADS * VD, D), (2 * HEADS * VD) ** -0.5, 0.1875, ((0, 4),)),
        "norm_gain": jnp.clip(1.0 + 0.18 * jax.random.normal(streams_of[11], (D,), jnp.float32), 0.1, 1.9),
        "w_gate": scatter_about(streams_of[12], (D, FF), D ** -0.5, 0.125, ((0, 8), (1, 4))),
        "w_up": scatter_about(streams_of[13], (D, FF), D ** -0.5, 0.125, ((0, 8), (1, 4))),
        "w_down": scatter_about(streams_of[14], (FF, D), (FF // 8) ** -0.5, 0.21875, ((0, 4), (1, 8))),
    }


eps_norm = 1e-06
head_scale = 0.8

def group_attend(queries, keys, values, lambdas, gain, width):
    total = queries.shape[0]
    heads = lambdas.shape[0]
    block = math.gcd(total, 512)
    query_blocks = queries.reshape(total // block, block, heads, 2, width)
    key_rows = keys.reshape(total, heads, 2, width).astype(jnp.float32)
    value_rows = values.reshape(total, heads, values.shape[1] // heads).astype(jnp.float32)

    def one_block(query_block):
        scores = jnp.einsum('qhme,khme->mhqk', query_block.astype(jnp.float32), key_rows) * width ** (-0.5)
        peak = lax.optimization_barrier(jnp.max(scores, axis=-1, keepdims=True))
        weights = jnp.exp(scores - peak)
        denom = lax.optimization_barrier(jnp.sum(weights, axis=-1))
        rounded = lax.optimization_barrier(weights.astype(jnp.bfloat16)).astype(jnp.float32)
        numer = jnp.einsum('mhqk,khv->mhqv', rounded, value_rows)
        ratio = numer / denom[..., None]
        mixed = ratio[0] - lambdas[:, None, None] * ratio[1]
        inverse = lax.rsqrt(lax.optimization_barrier(jnp.mean(mixed * mixed, axis=-1, keepdims=True)) + eps_norm)
        normed = mixed * inverse * gain * head_scale
        return jnp.transpose(normed, (1, 0, 2)).reshape(block, -1).astype(jnp.bfloat16)
    return lax.map(one_block, query_blocks).reshape(total, -1)

def reference(residual, queries_a, keys_a, values_a, queries_b, keys_b, values_b, mix_lambda, head_gain, out_a, out_b, norm_gain, w_gate, w_up, w_down):
    heads_a = group_attend(queries_a, keys_a, values_a, mix_lambda[0], head_gain[0], QA)
    heads_b = group_attend(queries_b, keys_b, values_b, mix_lambda[1], head_gain[1], QB)
    total = residual.shape[0]
    block = math.gcd(total, 2048)
    count = total // block

    def row_block(inputs):
        residual_rows, first_rows, second_rows = inputs
        mixed = jnp.dot(first_rows, out_a, preferred_element_type=jnp.float32)
        mixed = mixed + jnp.dot(second_rows, out_b, preferred_element_type=jnp.float32)
        summed = residual_rows.astype(jnp.float32) + mixed
        inverse = lax.rsqrt(lax.optimization_barrier(jnp.mean(summed * summed, axis=-1, keepdims=True)) + eps_norm)
        normed = (summed * inverse * norm_gain).astype(jnp.bfloat16)
        gate = jnp.dot(normed, w_gate, preferred_element_type=jnp.float32)
        upward = jnp.dot(normed, w_up, preferred_element_type=jnp.float32)
        hidden = (jax.nn.silu(gate) * upward).astype(jnp.bfloat16)
        channel = jnp.dot(hidden, w_down, preferred_element_type=jnp.float32)
        return (summed + 0.5 * channel).astype(jnp.bfloat16)
    result = lax.map(row_block, (residual.reshape(count, block, -1), heads_a.reshape(count, block, -1), heads_b.reshape(count, block, -1)))
    return result.reshape(total, -1)
```

```python
import functools
import math

import jax
import jax.numpy as jnp
from jax import lax
from jax.experimental import pallas as pl
from jax.experimental.pallas import tpu as pltpu
from jax.sharding import PartitionSpec as P

eps_norm = 1e-06
head_scale = 0.8
MESH = pl.DeviceIdType.MESH
CHUNKS = 4
NT = (((1,), (1,)), ((), ()))


def flip(index, bit):
    return index + bit - 2 * bit * ((index // bit) % 2)


def flip_all(index, mask):
    bit = 1
    while bit <= mask:
        if mask & bit:
            index = flip(index, bit)
        bit *= 2
    return index


def kernel(
    n, tp, residual_in, qa, ka, va, qb, kb, vb, lam, gain, oa, ob, ngain, wg_in, wu_in, wd, out,
    kv_all, wg_turn, wu_turn, wg_all, wu_all, wd_all, out_all, heads_all, summed, normed, hidden, channel, near_out,
    near_in, far_out, far_in, mate_out, mate_in, mine, turned, residual, wg, wu, query_a, query_b, mix_out, mix, local_sem, twin_send, twin_recv, chain_send,
    kv_recv, cross_recv, cube_send, cube_recv, out_send, out_recv, head_send,
    head_recv, swap_sem, norm_send, norm_recv, red_send, red_recv,
):
    rows, width = residual.shape
    heads = lam.shape[1]
    sa, sb = qa.shape[1] // (2 * heads), qb.shape[1] // (2 * heads)
    vd = va.shape[1] // heads
    hv = heads * vd
    total = n * rows
    block = math.gcd(rows, 1 << min(7, ((1 << 19) // total).bit_length() - 1))
    nb = rows // block
    share = width // tp
    depth, units = wg.shape
    half = units // 2
    sp_me, tp_me = lax.axis_index("sp"), lax.axis_index("tp")
    line, length = sp_me // 2, n // 2
    core = tp_me % 2
    sp_twin, tp_twin = 2 * line + core, 2 * (tp_me // 2) + sp_me % 2
    apart = sp_me % 2 != core
    peers = [(tp_me + k) % tp for k in range(1, tp)]
    pair = n // 2
    side = (sp_me // pair) % 2
    mate = flip(sp_me, pair)
    bits = [pair]
    while bits[-1] > 1:
        bits.append(bits[-1] // 2)
    last = len(bits) - 1

    ck, cv = ka.shape[1], ka.shape[1] + kb.shape[1]
    part = rows // CHUNKS

    def strips(src, low, size):
        return [
            (src.at[pl.ds(c * part, part)], kv_all.at[sp_me, pl.ds(c * part, part), pl.ds(low, size)])
            for c in range(CHUNKS)
        ]

    pieces = [strips(ka, 0, ck), strips(kb, ck, kb.shape[1]), strips(va, cv, hv), strips(vb, cv + hv, hv)]
    swaps = [pieces[i][c] for c in range(CHUNKS) for i in range(4)]
    others = len(swaps)
    swaps += [(qa, query_a), (qb, query_b), (mix_out, mix), (mine, turned)]

    def twin(i):
        src, dst = swaps[i]
        return pltpu.make_async_remote_copy(
            src_ref=src, dst_ref=dst, send_sem=twin_send.at[i], recv_sem=twin_recv.at[i],
            device_id={"sp": sp_twin, "tp": tp_twin}, device_id_type=MESH,
        )

    def twin_local(i):
        src, dst = swaps[i]
        return pltpu.make_async_copy(src, dst, twin_recv.at[i])

    def twin_start(chosen):
        @pl.when(apart)
        def _():
            for i in chosen:
                twin(i).start()

        @pl.when(jnp.logical_not(apart))
        def _():
            for i in chosen:
                twin_local(i).start()

    def twin_wait(chosen):
        @pl.when(apart)
        def _():
            for i in chosen:
                twin(i).wait_recv()

        @pl.when(jnp.logical_not(apart))
        def _():
            for i in chosen:
                twin_local(i).wait()

    own = [
        (wg_in, wg),
        (wu_in, wu),
        (wd.at[pl.ds(pl.multiple_of(side * half, half), half)], wd_all.at[sp_me]),
        (oa, out_all.at[tp_me, pl.ds(0, hv)]),
        (ob, out_all.at[tp_me, pl.ds(hv, hv)]),
        (residual_in, residual),
    ]
    copies = [pltpu.make_async_copy(s, d, local_sem.at[i]) for i, (s, d) in enumerate(own)]
    for c in copies:
        c.start()

    barrier = pltpu.get_barrier_semaphore()
    for bit in bits:
        pl.semaphore_signal(barrier, inc=1, device_id={"sp": flip(sp_me, bit)}, device_id_type=MESH)
    for peer in peers:
        pl.semaphore_signal(barrier, inc=1, device_id={"tp": peer}, device_id_type=MESH)

    @pl.when(line > 0)
    def _():
        pl.semaphore_signal(barrier, inc=1, device_id={"sp": sp_me - 2}, device_id_type=MESH)

    @pl.when(line < length - 1)
    def _():
        pl.semaphore_signal(barrier, inc=1, device_id={"sp": sp_me + 2}, device_id_type=MESH)

    @pl.when(apart)
    def _():
        pl.semaphore_signal(
            barrier, inc=1, device_id={"sp": sp_twin, "tp": tp_twin}, device_id_type=MESH
        )

    for g in range(2):
        for h in range(heads):
            at = g * heads + h
            mix_out[at : at + 1, :] = jnp.full((1, mix_out.shape[1]), lam[g, h], jnp.float32)
    greeted = len(bits) + len(peers) + (line > 0).astype(jnp.int32) + (line < length - 1).astype(jnp.int32)
    pl.semaphore_wait(barrier, greeted + apart.astype(jnp.int32))

    towards = (sp_me + 2, sp_me - 2)

    def block_of(c, at, who):
        return kv_all.at[2 * at + who, pl.ds(c * part, part)]

    def chain(c, d, at):
        view = block_of(c, at, core)
        return pltpu.make_async_remote_copy(
            src_ref=view, dst_ref=view, send_sem=chain_send.at[c, d, at], recv_sem=kv_recv.at[c, at],
            device_id={"sp": towards[d]}, device_id_type=MESH,
        )

    def cross(c, at, arriving=False):
        view = block_of(c, at, 1 - core if arriving else core)
        return pltpu.make_async_remote_copy(
            src_ref=view, dst_ref=view, send_sem=chain_send.at[c, 2, at], recv_sem=cross_recv.at[c, at],
            device_id={"tp": flip(tp_me, 1)}, device_id_type=MESH,
        )

    rest = (line < length - 1, line > 0)

    def onward(c, d, at):
        @pl.when(rest[d])
        def _():
            chain(c, d, at).start()

    twin_start(range(others + 3))

    tp_bits = []
    while (tp >> (len(tp_bits) + 1)) > 0:
        tp_bits.append(tp >> (len(tp_bits) + 1))
    tp_order, tp_came = [0], {}
    for k, bit in enumerate(tp_bits):
        for held in list(tp_order):
            tp_came[held | bit] = (held, k)
            tp_order.append(held | bit)

    def tp_copy(gather, held, k, arriving):
        view, first, sends, recvs = gather
        mask = held | tp_bits[k]
        dst = view(flip_all(tp_me, mask if arriving else held))
        return pltpu.make_async_remote_copy(
            src_ref=first if first is not None and held == 0 and not arriving else dst, dst_ref=dst,
            send_sem=sends.at[mask - 1], recv_sem=recvs.at[mask - 1],
            device_id={"tp": flip(tp_me, tp_bits[k])}, device_id_type=MESH,
        )

    def tp_forward(gather, mask):
        for k in range(tp_came[mask][1] + 1 if mask else 0, len(tp_bits)):
            tp_copy(gather, mask, k, False).start()

    def tp_arrive(gather, masks):
        for mask in masks:
            held, k = tp_came[mask]
            tp_copy(gather, held, k, True).wait_recv()
            tp_forward(gather, mask)

    def tp_drain(gather):
        for mask in tp_order[1:]:
            held, k = tp_came[mask]
            tp_copy(gather, held, k, False).wait_send()

    out_gather = (lambda slot: out_all.at[slot], None, out_send, out_recv)
    head_gather = (lambda slot: heads_all.at[slot], turned, head_send, head_recv)
    for c in copies[:5]:
        c.wait()
    tp_forward(out_gather, 0)

    tile = math.gcd(units, 128)

    def turn(i):
        at = pl.ds(pl.multiple_of(i * tile, tile), tile)
        wg_turn[at, :] = wg[:, at].T
        wu_turn[at, :] = wu[:, at].T

    def turn_all(i, _):
        turn(i)
        return 0

    lax.fori_loop(0, units // tile, turn_all, 0)
    wg_all[sp_me] = wg_turn[pl.ds(pl.multiple_of(side * half, half), half), :]
    wu_all[sp_me] = wu_turn[pl.ds(pl.multiple_of(side * half, half), half), :]

    gathered = (wg_all, wu_all, wd_all)
    whole = (wg_turn, wu_turn, wd)

    def cube(a, held, k, arriving):
        mask = held | bits[k]
        owner = flip_all(sp_me, mask if arriving else held)
        dst = gathered[a].at[owner]
        src = dst
        if k == 0 and not arriving:
            src = whole[a].at[pl.ds(pl.multiple_of((1 - side) * half, half), half)]
        return pltpu.make_async_remote_copy(
            src_ref=src, dst_ref=dst,
            send_sem=cube_send.at[a, mask], recv_sem=cube_recv.at[a, mask],
            device_id={"sp": flip(sp_me, bits[k])}, device_id_type=MESH,
        )

    order = [0]
    came = {}
    for k, bit in enumerate(bits):
        for held in list(order):
            came[held | bit] = (held, k)
            order.append(held | bit)

    def forward(a, mask, least=0, most=len(bits)):
        first = came[mask][1] + 1 if mask else 0
        for k in range(max(first, least), most):
            cube(a, mask, k, False).start()

    def arrive(a, mask):
        held, k = came[mask]
        cube(a, held, k, True).wait_recv()
        forward(a, mask)

    events = []
    for k in range(len(bits)):
        for a in range(3):
            for mask in order[1:]:
                if came[mask][1] == k:
                    events.append((a, mask))

    def take(chosen):
        for a, mask in chosen:
            arrive(a, mask)
            events.remove((a, mask))

    def pick(a, low, high, paired=None):
        return [
            (b, mask) for b, mask in events
            if b == a and low <= came[mask][1] < high and (paired is None or bool(mask & pair) == paired)
        ]

    def own_rows_out():
        for a in (2, 0, 1):
            forward(a, 0, least=last)

    for c in range(CHUNKS):
        twin_wait(range(4 * c, 4 * c + 4))
        for d in range(2):
            onward(c, d, line)
        cross(c, line).start()

    @pl.when(apart)
    def _():
        own_rows_out()

    forward(0, 0, least=1, most=last)
    outer = jnp.logical_or(line < length // 4, line >= length - length // 4)

    def to_mate(chosen, where):
        @pl.when(where)
        def _():
            for a in chosen:
                forward(a, 0, most=1)

    to_mate([0], outer)
    for t in range(1, length):
        for d in range(2):
            at = line - t if d == 0 else line + t

            @pl.when(at >= 0 if d == 0 else at < length)
            def _():
                for c in range(CHUNKS):
                    chain(c, d, at).wait_recv()
                    onward(c, d, at)
                    cross(c, at).start()

        if t == 1:
            @pl.when(jnp.logical_not(apart))
            def _():
                own_rows_out()

        if t <= 2:
            to_mate([t], outer)
        if t == min(2, length - 1):
            take(pick(0, 1, last, False))
    for a in (1, 2):
        forward(a, 0, least=1, most=last)
    twin_wait(range(others, others + 3))
    for c in range(CHUNKS):
        for at in range(length):
            cross(c, at, True).wait_recv()

    def attend(group, r):
        queries = query_a if group == 0 else query_b
        size = sa if group == 0 else sb
        base = 0 if group == 0 else ck
        factor = size ** (-0.5) * math.log2(math.e)
        at = pl.ds(pl.multiple_of(r * block, block), block)
        for h in range(heads):
            start = 2 * h * size
            query = queries[at, start : start + 2 * size]
            value = kv_all[:, :, cv + group * hv + h * vd : cv + group * hv + (h + 1) * vd].reshape(total, vd)
            lanes = lax.broadcasted_iota(jnp.int32, query.shape, 1)
            ratios = []
            for j in range(2):
                if size % 128 == 0:
                    q = query[:, j * size : (j + 1) * size]
                    low = base + start + j * size
                    key = kv_all[:, :, low : low + size].reshape(total, size)
                else:
                    q = jnp.where(lanes // size == j, query, jnp.zeros_like(query))
                    low = base + start
                    key = kv_all[:, :, low : low + 2 * size].reshape(total, 2 * size)
                scores = lax.dot_general(q, key, NT, preferred_element_type=jnp.float32)
                peak = jnp.max(scores, axis=1, keepdims=True)
                weights = jnp.exp2((scores - peak) * factor)
                denom = jnp.sum(weights, axis=1, keepdims=True)
                numer = jnp.dot(weights.astype(jnp.bfloat16), value, preferred_element_type=jnp.float32)
                ratios.append(numer / denom)
            mixed = ratios[0] - mix[group * heads + h : group * heads + h + 1, :vd] * ratios[1]
            inverse = lax.rsqrt(jnp.mean(mixed * mixed, axis=-1, keepdims=True) + eps_norm)
            result = mixed * inverse * gain[group : group + 1, :] * head_scale
            col = group * hv + h * vd
            mine[at, col : col + vd] = result.astype(jnp.bfloat16)

    for group in range(2):
        def body(r, _, group=group):
            attend(group, r)
            return 0

        lax.fori_loop(0, nb, body, 0)
        if group == 0:
            tp_arrive(out_gather, tp_order[1:-1])

    twin_start([others + 3])
    take(pick(1, 1, last, False))
    to_mate(range(3), jnp.logical_not(outer))
    tp_arrive(out_gather, tp_order[-1:])
    twin_wait([others + 3])
    tp_forward(head_gather, 0)
    take(pick(0, 0, 1))
    take(pick(2, 1, last, False))
    tp_arrive(head_gather, tp_order[1:])
    heads_all[tp_me] = turned[...]

    tall = math.gcd(rows, 128)
    count = rows // tall

    def swap(r, arriving):
        there = 1 - side if arriving else side
        view = normed.at[there, tp_me, pl.ds(pl.multiple_of(r * tall, tall), tall)]
        return pltpu.make_async_remote_copy(
            src_ref=view, dst_ref=view, send_sem=swap_sem.at[0, r], recv_sem=swap_sem.at[1, r],
            device_id={"sp": mate}, device_id_type=MESH,
        )

    def project(r, _):
        @pl.when(r > 0)
        def _():
            swap(r - 1, False).start()

        at = pl.ds(pl.multiple_of(r * tall, tall), tall)
        acc = residual[at, :].astype(jnp.float32)
        for d in range(tp):
            acc = acc + jnp.dot(heads_all[d, at, :], out_all[d], preferred_element_type=jnp.float32)
        inverse = lax.rsqrt(jnp.mean(acc * acc, axis=-1, keepdims=True) + eps_norm)
        scaled = (acc * inverse * ngain[...]).astype(jnp.bfloat16)
        for d in range(tp):
            normed[side, d, at, :] = scaled[:, d * share : (d + 1) * share]

            @pl.when(d == tp_me)
            def _():
                summed[at, :] = acc[:, d * share : (d + 1) * share]

        return 0

    copies[5].wait()
    lax.fori_loop(0, count, project, 0)
    swap(count - 1, False).start()
    norm_gathers = [
        (
            lambda slot, r=r: normed.at[1 - side, slot, pl.ds(r * tall, tall)], None,
            norm_send.at[r], norm_recv.at[r],
        )
        for r in range(count)
    ]
    take(pick(1, 0, 1))
    take(pick(0, 1, last))
    for r in range(count):
        swap(r, True).wait_recv()
        tp_forward(norm_gathers[r], 0)
    take(pick(1, 1, last))
    take(pick(2, 0, 1))
    take(pick(0, last, last + 1))
    take(pick(1, last, last + 1))

    step_cols = share // depth

    def feed(where):
        gate = jnp.zeros((rows, half), jnp.float32)
        upward = jnp.zeros((rows, half), jnp.float32)
        for s in range(n):
            low = (s % step_cols) * depth
            x = normed[where, s // step_cols, :, low : low + depth]
            gate = gate + lax.dot_general(x, wg_all[s], NT, preferred_element_type=jnp.float32)
            upward = upward + lax.dot_general(x, wu_all[s], NT, preferred_element_type=jnp.float32)
        hidden[where] = (gate / (1.0 + jnp.exp(-gate)) * upward).astype(jnp.bfloat16)

    def feed_one(i, _):
        @pl.when(i == 1)
        def _():
            for r in range(count):
                tp_arrive(norm_gathers[r], tp_order[1:])

        feed((side + i) % 2)
        return 0

    lax.fori_loop(0, 2, feed_one, 0)
    cols = wd_all.shape[2]
    ratio = share // cols
    east = tp_me // 2

    def hand(src, dst, group, index, **target):
        return pltpu.make_async_remote_copy(
            src_ref=src, dst_ref=dst, send_sem=red_send.at[group, index], recv_sem=red_recv.at[group, index],
            device_id=target, device_id_type=MESH,
        )

    def near(index):
        return hand(near_out.at[index], near_in.at[index], 0, index, tp=flip(tp_me, 1))

    def far(index):
        return hand(far_out.at[index], far_in.at[index], 1, index, tp=flip(tp_me, 2))

    def across(index):
        return hand(mate_out.at[index], mate_in.at[index], 2, index, sp=mate)

    def slab_of(mask):
        slab = flip_all(sp_me, mask)
        target = slab // ratio
        return slab, target, (target // 2) * ratio + slab % ratio, slab % ratio

    def product(where, slab):
        return jnp.dot(hidden[where], wd_all[slab], preferred_element_type=jnp.float32)

    def give(mask):
        slab, target, index, _ = slab_of(mask)

        @pl.when(target % 2 != core)
        def _():
            def one(where, _):
                near_out[index, where] = product(where, slab).astype(jnp.bfloat16)
                return 0

            lax.fori_loop(0, 2, one, 0)
            near(index).start()

    def gain_near(mask):
        slab, target, index, low = slab_of(mask)

        @pl.when(target % 2 == core)
        def _():
            near(index).wait_recv()

            @pl.when(target // 2 == east)
            def _():
                def one(where, _):
                    channel[low, where] = product(where, slab) + near_in[index, where].astype(jnp.float32)
                    return 0

                lax.fori_loop(0, 2, one, 0)

            @pl.when(target // 2 != east)
            def _():
                def one(where, _):
                    both = product(where, slab) + near_in[index, where].astype(jnp.float32)
                    far_out[low, where] = both.astype(jnp.bfloat16)
                    return 0

                lax.fori_loop(0, 2, one, 0)
                far(low).start()

    def gain_far(mask):
        slab, target, index, low = slab_of(mask)

        @pl.when(target == tp_me)
        def _():
            far(low).wait_recv()
            channel[low, 1 - side] = channel[low, 1 - side] + far_in[low, 1 - side].astype(jnp.float32)
            mate_out[low] = channel[low, 1 - side].astype(jnp.bfloat16)
            across(low).start()
            channel[low, side] = channel[low, side] + far_in[low, side].astype(jnp.float32)

    steps = [m ^ p for m in order if not m & pair for p in (0, pair)]
    for i in range(len(steps) + 2):
        if i < len(steps):
            held = steps[i]
            if i == 0:
                take(pick(2, 1, last))
            take([e for e in events if e[1] == held])
            give(held)
        if 0 <= i - 1 < len(steps):
            gain_near(steps[i - 1])
        if 0 <= i - 2 < len(steps):
            gain_far(steps[i - 2])
    for low in range(ratio):
        across(low).wait_recv()
        final = channel[low, side] + mate_in[low].astype(jnp.float32)
        at = slice(low * cols, (low + 1) * cols)
        out[:, at] = (summed[:, at] + 0.5 * final).astype(jnp.bfloat16)

    for low in range(ratio):
        across(low).wait_send()
        far(low).wait_send()
    for index in range(n // 2):
        near(index).wait_send()
    for r in range(count):
        swap(r, False).wait_send()
    for gather in [out_gather, head_gather] + norm_gathers:
        tp_drain(gather)
    for a in range(3):
        for mask in order[1:]:
            held, k = came[mask]
            cube(a, held, k, False).wait_send()

    @pl.when(apart)
    def _():
        for i in range(len(swaps)):
            twin(i).wait_send()

    for c in range(CHUNKS):
        for at in range(length):
            cross(c, at).wait_send()
            for d in range(2):
                @pl.when(jnp.logical_and(rest[d], at <= line if d == 0 else at >= line))
                def _():
                    chain(c, d, at).wait_send()


def local(
    n, tp, residual, queries_a, keys_a, values_a, queries_b, keys_b, values_b, mix_lambda, head_gain,
    out_a, out_b, norm_gain, w_gate, w_up, w_down,
):
    rows, width = residual.shape
    share = width // tp
    units = w_gate.shape[1]
    hv = out_a.shape[0]
    cols = w_down.shape[1]
    tall = math.gcd(rows, 128)
    span = keys_a.shape[1] + keys_b.shape[1] + values_a.shape[1] + values_b.shape[1]
    vmem, anywhere = pl.BlockSpec(memory_space=pltpu.VMEM), pl.BlockSpec(memory_space=pl.ANY)
    smem = pl.BlockSpec(memory_space=pltpu.SMEM)
    bf16, f32 = jnp.bfloat16, jnp.float32
    dma = pltpu.SemaphoreType.DMA
    return pl.pallas_call(
        functools.partial(kernel, n, tp),
        out_shape=jax.ShapeDtypeStruct((rows, share), bf16),
        in_specs=[
            anywhere, anywhere, anywhere, anywhere, anywhere, anywhere, anywhere, smem, vmem,
            anywhere, anywhere, vmem, anywhere, anywhere, anywhere,
        ],
        out_specs=vmem,
        scratch_shapes=[
            pltpu.VMEM((n, rows, span), bf16),
            pltpu.VMEM((units, w_gate.shape[0]), bf16),
            pltpu.VMEM((units, w_gate.shape[0]), bf16),
            pltpu.VMEM((n, units // 2, w_gate.shape[0]), bf16),
            pltpu.VMEM((n, units // 2, w_gate.shape[0]), bf16),
            pltpu.VMEM((n, units // 2, w_down.shape[1]), bf16),
            pltpu.VMEM((tp, 2 * hv, width), bf16),
            pltpu.VMEM((tp, rows, 2 * hv), bf16),
            pltpu.VMEM((rows, share), f32),
            pltpu.VMEM((2, tp, rows, share), bf16),
            pltpu.VMEM((2, rows, units // 2), bf16),
            pltpu.VMEM((n // tp, 2, rows, cols), f32),
            pltpu.VMEM((n // 2, 2, rows, cols), bf16),
            pltpu.VMEM((n // 2, 2, rows, cols), bf16),
            pltpu.VMEM((n // tp, 2, rows, cols), bf16),
            pltpu.VMEM((n // tp, 2, rows, cols), bf16),
            pltpu.VMEM((n // tp, rows, cols), bf16),
            pltpu.VMEM((n // tp, rows, cols), bf16),
            pltpu.VMEM((rows, 2 * hv), bf16),
            pltpu.VMEM((rows, 2 * hv), bf16),
            pltpu.VMEM(residual.shape, bf16),
            pltpu.VMEM(w_gate.shape, bf16),
            pltpu.VMEM(w_up.shape, bf16),
            pltpu.VMEM(queries_a.shape, bf16),
            pltpu.VMEM(queries_b.shape, bf16),
            pltpu.VMEM((8 * -(-mix_lambda.size // 8), hv), f32),
            pltpu.VMEM((8 * -(-mix_lambda.size // 8), hv), f32),
            dma((6,)),
            dma((4 * CHUNKS + 4,)),
            dma((4 * CHUNKS + 4,)),
            dma((CHUNKS, 3, n // 2)),
            dma((CHUNKS, n // 2)),
            dma((CHUNKS, n // 2)),
            dma((3, n)),
            dma((3, n)),
            dma((tp - 1,)),
            dma((tp - 1,)),
            dma((tp - 1,)),
            dma((tp - 1,)),
            dma((2, rows // tall)),
            dma((rows // tall, tp - 1)),
            dma((rows // tall, tp - 1)),
            dma((3, n // 2)),
            dma((3, n // 2)),
        ],
        compiler_params=pltpu.CompilerParams(
            collective_id=0, has_side_effects=True, vmem_limit_bytes=63 * 1024 * 1024
        ),
        name="layer",
    )(
        residual, queries_a, keys_a, values_a, queries_b, keys_b, values_b, mix_lambda, head_gain,
        out_a, out_b, norm_gain.reshape(1, -1), w_gate, w_up, w_down,
    )


def solution(mesh):
    in_specs = (
        P("sp", None),
        P("sp", "tp"),
        P("sp", "tp"),
        P("sp", "tp"),
        P("sp", "tp"),
        P("sp", "tp"),
        P("sp", "tp"),
        P(None, "tp"),
        P(),
        P("tp", None),
        P("tp", None),
        P(),
        P("sp", "tp"),
        P("sp", "tp"),
        P("tp", "sp"),
    )
    body = functools.partial(local, mesh.shape["sp"], mesh.shape["tp"])
    return jax.shard_map(body, mesh=mesh, in_specs=in_specs, out_specs=P("sp", "tp"), check_vma=False)
```

```python
import functools
import math

import jax
import jax.numpy as jnp
from jax import lax
from jax.experimental import pallas as pl
from jax.experimental.pallas import tpu as pltpu
from jax.sharding import PartitionSpec as P

eps_norm = 1e-06
head_scale = 0.8
MESH = pl.DeviceIdType.MESH
CHUNKS = 4
NT = (((1,), (1,)), ((), ()))


def flip(index, bit):
    return index + bit - 2 * bit * ((index // bit) % 2)


def flip_all(index, mask):
    bit = 1
    while bit <= mask:
        if mask & bit:
            index = flip(index, bit)
        bit *= 2
    return index


def kernel(
    n, tp, residual_in, qa, ka, va, qb, kb, vb, lam, gain, oa, ob, ngain, wg_in, wu_in, wd, out,
    kv_all, wg_turn, wu_turn, wg_all, wu_all, wd_all, out_all, heads_all, summed, normed, hidden, channel, near_out,
    near_in, far_out, far_in, mate_out, mate_in, mine, turned, residual, wg, wu, query_a, query_b, mix_out, mix, lend_send, lend_recv, local_sem, twin_send, twin_recv, chain_send,
    kv_recv, cross_recv, cube_send, cube_recv, out_send, out_recv, head_send,
    head_recv, swap_sem, norm_send, norm_recv, red_send, red_recv,
):
    rows, width = residual.shape
    heads = lam.shape[1]
    sa, sb = qa.shape[1] // (2 * heads), qb.shape[1] // (2 * heads)
    vd = va.shape[1] // heads
    hv = heads * vd
    total = n * rows
    block = math.gcd(rows, 1 << min(7, ((1 << 19) // total).bit_length() - 1))
    nb = rows // block
    share = width // tp
    depth, units = wg.shape
    half = units // 2
    sp_me, tp_me = lax.axis_index("sp"), lax.axis_index("tp")
    line, length = sp_me // 2, n // 2
    core = tp_me % 2
    sp_twin, tp_twin = 2 * line + core, 2 * (tp_me // 2) + sp_me % 2
    apart = sp_me % 2 != core
    peers = [(tp_me + k) % tp for k in range(1, tp)]
    pair = n // 2
    side = (sp_me // pair) % 2
    mate = flip(sp_me, pair)
    bits = [pair]
    while bits[-1] > 1:
        bits.append(bits[-1] // 2)
    last = len(bits) - 1

    ck, cv = ka.shape[1], ka.shape[1] + kb.shape[1]
    part = rows // CHUNKS

    def strips(src, low, size):
        return [
            (src.at[pl.ds(c * part, part)], kv_all.at[sp_me, pl.ds(c * part, part), pl.ds(low, size)])
            for c in range(CHUNKS)
        ]

    pieces = [strips(ka, 0, ck), strips(kb, ck, kb.shape[1]), strips(va, cv, hv), strips(vb, cv + hv, hv)]
    swaps = [pieces[i][c] for c in range(CHUNKS) for i in range(4)]
    others = len(swaps)
    swaps += [(qa, query_a.at[0]), (qb, query_b.at[0]), (mix_out, mix), (mine.at[0], turned)]

    def twin(i):
        src, dst = swaps[i]
        return pltpu.make_async_remote_copy(
            src_ref=src, dst_ref=dst, send_sem=twin_send.at[i], recv_sem=twin_recv.at[i],
            device_id={"sp": sp_twin, "tp": tp_twin}, device_id_type=MESH,
        )

    def twin_local(i):
        src, dst = swaps[i]
        return pltpu.make_async_copy(src, dst, twin_recv.at[i])

    def twin_start(chosen):
        @pl.when(apart)
        def _():
            for i in chosen:
                twin(i).start()

        @pl.when(jnp.logical_not(apart))
        def _():
            for i in chosen:
                twin_local(i).start()

    def twin_wait(chosen):
        @pl.when(apart)
        def _():
            for i in chosen:
                twin(i).wait_recv()

        @pl.when(jnp.logical_not(apart))
        def _():
            for i in chosen:
                twin_local(i).wait()

    own = [
        (wg_in, wg),
        (wu_in, wu),
        (wd.at[pl.ds(pl.multiple_of(side * half, half), half)], wd_all.at[sp_me]),
        (oa, out_all.at[tp_me, pl.ds(0, hv)]),
        (ob, out_all.at[tp_me, pl.ds(hv, hv)]),
        (residual_in, residual),
    ]
    copies = [pltpu.make_async_copy(s, d, local_sem.at[i]) for i, (s, d) in enumerate(own)]
    for c in copies:
        c.start()

    barrier = pltpu.get_barrier_semaphore()
    for bit in bits:
        pl.semaphore_signal(barrier, inc=1, device_id={"sp": flip(sp_me, bit)}, device_id_type=MESH)
    for peer in peers:
        pl.semaphore_signal(barrier, inc=1, device_id={"tp": peer}, device_id_type=MESH)

    @pl.when(line > 0)
    def _():
        pl.semaphore_signal(barrier, inc=1, device_id={"sp": sp_me - 2}, device_id_type=MESH)

    @pl.when(line < length - 1)
    def _():
        pl.semaphore_signal(barrier, inc=1, device_id={"sp": sp_me + 2}, device_id_type=MESH)

    @pl.when(apart)
    def _():
        pl.semaphore_signal(
            barrier, inc=1, device_id={"sp": sp_twin, "tp": tp_twin}, device_id_type=MESH
        )

    for g in range(2):
        for h in range(heads):
            at = g * heads + h
            mix_out[at : at + 1, :] = jnp.full((1, mix_out.shape[1]), lam[g, h], jnp.float32)
    greeted = len(bits) + len(peers) + (line > 0).astype(jnp.int32) + (line < length - 1).astype(jnp.int32)
    pl.semaphore_wait(barrier, greeted + apart.astype(jnp.int32))

    towards = (sp_me + 2, sp_me - 2)

    def block_of(c, at, who):
        return kv_all.at[2 * at + who, pl.ds(c * part, part)]

    def chain(c, d, at):
        view = block_of(c, at, core)
        return pltpu.make_async_remote_copy(
            src_ref=view, dst_ref=view, send_sem=chain_send.at[c, d, at], recv_sem=kv_recv.at[c, at],
            device_id={"sp": towards[d]}, device_id_type=MESH,
        )

    def cross(c, at, arriving=False):
        view = block_of(c, at, 1 - core if arriving else core)
        return pltpu.make_async_remote_copy(
            src_ref=view, dst_ref=view, send_sem=chain_send.at[c, 2, at], recv_sem=cross_recv.at[c, at],
            device_id={"tp": flip(tp_me, 1)}, device_id_type=MESH,
        )

    quarter = length // 4
    outer = jnp.logical_or(line < quarter, line >= length - quarter)
    inner = jnp.logical_not(outer)
    rest = (line + 1 < length - quarter, line - 1 >= quarter)
    reach = (line < length - quarter, line >= quarter)
    lender = flip(sp_me, n // 4)
    loans = [(query_a.at[0], query_a.at[1]), (query_b.at[0], query_b.at[1]), (mine.at[1], mine.at[0])]

    def lend(i):
        src, dst = loans[i]
        return pltpu.make_async_remote_copy(
            src_ref=src, dst_ref=dst, send_sem=lend_send.at[i], recv_sem=lend_recv.at[i],
            device_id={"sp": lender}, device_id_type=MESH,
        )

    def onward(c, d, at):
        @pl.when(rest[d])
        def _():
            chain(c, d, at).start()

    twin_start(range(others + 3))

    tp_bits = []
    while (tp >> (len(tp_bits) + 1)) > 0:
        tp_bits.append(tp >> (len(tp_bits) + 1))
    tp_order, tp_came = [0], {}
    for k, bit in enumerate(tp_bits):
        for held in list(tp_order):
            tp_came[held | bit] = (held, k)
            tp_order.append(held | bit)

    def tp_copy(gather, held, k, arriving):
        view, first, sends, recvs = gather
        mask = held | tp_bits[k]
        dst = view(flip_all(tp_me, mask if arriving else held))
        return pltpu.make_async_remote_copy(
            src_ref=first if first is not None and held == 0 and not arriving else dst, dst_ref=dst,
            send_sem=sends.at[mask - 1], recv_sem=recvs.at[mask - 1],
            device_id={"tp": flip(tp_me, tp_bits[k])}, device_id_type=MESH,
        )

    def tp_forward(gather, mask):
        for k in range(tp_came[mask][1] + 1 if mask else 0, len(tp_bits)):
            tp_copy(gather, mask, k, False).start()

    def tp_arrive(gather, masks):
        for mask in masks:
            held, k = tp_came[mask]
            tp_copy(gather, held, k, True).wait_recv()
            tp_forward(gather, mask)

    def tp_drain(gather):
        for mask in tp_order[1:]:
            held, k = tp_came[mask]
            tp_copy(gather, held, k, False).wait_send()

    out_gather = (lambda slot: out_all.at[slot], None, out_send, out_recv)
    head_gather = (lambda slot: heads_all.at[slot], turned, head_send, head_recv)
    for c in copies[:5]:
        c.wait()
    tp_forward(out_gather, 0)

    tile = math.gcd(units, 128)

    def turn(i):
        at = pl.ds(pl.multiple_of(i * tile, tile), tile)
        wg_turn[at, :] = wg[:, at].T
        wu_turn[at, :] = wu[:, at].T

    def turn_all(i, _):
        turn(i)
        return 0

    lax.fori_loop(0, units // tile, turn_all, 0)
    wg_all[sp_me] = wg_turn[pl.ds(pl.multiple_of(side * half, half), half), :]
    wu_all[sp_me] = wu_turn[pl.ds(pl.multiple_of(side * half, half), half), :]

    gathered = (wg_all, wu_all, wd_all)
    whole = (wg_turn, wu_turn, wd)

    def cube(a, held, k, arriving):
        mask = held | bits[k]
        owner = flip_all(sp_me, mask if arriving else held)
        dst = gathered[a].at[owner]
        src = dst
        if k == 0 and not arriving:
            src = whole[a].at[pl.ds(pl.multiple_of((1 - side) * half, half), half)]
        return pltpu.make_async_remote_copy(
            src_ref=src, dst_ref=dst,
            send_sem=cube_send.at[a, mask], recv_sem=cube_recv.at[a, mask],
            device_id={"sp": flip(sp_me, bits[k])}, device_id_type=MESH,
        )

    order = [0]
    came = {}
    for k, bit in enumerate(bits):
        for held in list(order):
            came[held | bit] = (held, k)
            order.append(held | bit)

    def forward(a, mask, least=0, most=len(bits)):
        first = came[mask][1] + 1 if mask else 0
        for k in range(max(first, least), most):
            cube(a, mask, k, False).start()

    def arrive(a, mask):
        held, k = came[mask]
        cube(a, held, k, True).wait_recv()
        forward(a, mask)

    events = []
    for k in range(len(bits)):
        for a in range(3):
            for mask in order[1:]:
                if came[mask][1] == k:
                    events.append((a, mask))

    def take(chosen):
        for a, mask in chosen:
            arrive(a, mask)
            events.remove((a, mask))

    def pick(a, low, high, paired=None):
        return [
            (b, mask) for b, mask in events
            if b == a and low <= came[mask][1] < high and (paired is None or bool(mask & pair) == paired)
        ]

    def own_rows_out():
        for a in (2, 0, 1):
            forward(a, 0, least=last)

    def over(c, at):
        @pl.when(inner)
        def _():
            cross(c, at).start()

    def to_mate(chosen, where):
        @pl.when(where)
        def _():
            for a in chosen:
                forward(a, 0, most=1)

    for c in range(CHUNKS):
        twin_wait(range(4 * c, 4 * c + 4))
        for d in range(2):
            onward(c, d, line)
        over(c, line)

    @pl.when(apart)
    def _():
        own_rows_out()

    forward(0, 0, least=1, most=last)
    twin_wait(range(others, others + 3))

    @pl.when(outer)
    def _():
        lend(0).start()
        lend(1).start()

    to_mate([0], outer)
    for t in range(1, length):
        for d in range(2):
            at = line - t if d == 0 else line + t

            @pl.when(jnp.logical_and(reach[d], at >= 0 if d == 0 else at < length))
            def _():
                for c in range(CHUNKS):
                    chain(c, d, at).wait_recv()
                    onward(c, d, at)
                    over(c, at)

        if t == 1:
            @pl.when(jnp.logical_not(apart))
            def _():
                own_rows_out()

    take(pick(0, 1, last, False))
    to_mate([0], inner)
    forward(1, 0, least=1, most=last)
    to_mate([1], outer)
    to_mate([1], inner)

    @pl.when(inner)
    def _():
        for c in range(CHUNKS):
            for at in range(length):
                cross(c, at, True).wait_recv()
        lend(0).wait_recv()
        lend(1).wait_recv()

    def attend(which, group, r):
        queries = query_a.at[which] if group == 0 else query_b.at[which]
        size = sa if group == 0 else sb
        base = 0 if group == 0 else ck
        factor = size ** (-0.5) * math.log2(math.e)
        at = pl.ds(pl.multiple_of(r * block, block), block)
        for h in range(heads):
            start = 2 * h * size
            query = queries[at, start : start + 2 * size]
            value = kv_all[:, :, cv + group * hv + h * vd : cv + group * hv + (h + 1) * vd].reshape(total, vd)
            lanes = lax.broadcasted_iota(jnp.int32, query.shape, 1)
            ratios = []
            for j in range(2):
                if size % 128 == 0:
                    q = query[:, j * size : (j + 1) * size]
                    low = base + start + j * size
                    key = kv_all[:, :, low : low + size].reshape(total, size)
                else:
                    q = jnp.where(lanes // size == j, query, jnp.zeros_like(query))
                    low = base + start
                    key = kv_all[:, :, low : low + 2 * size].reshape(total, 2 * size)
                scores = lax.dot_general(q, key, NT, preferred_element_type=jnp.float32)
                peak = jnp.max(scores, axis=1, keepdims=True)
                weights = jnp.exp2((scores - peak) * factor)
                denom = jnp.sum(weights, axis=1, keepdims=True)
                numer = jnp.dot(weights.astype(jnp.bfloat16), value, preferred_element_type=jnp.float32)
                ratios.append(numer / denom)
            mixed = ratios[0] - mix[group * heads + h : group * heads + h + 1, :vd] * ratios[1]
            inverse = lax.rsqrt(jnp.mean(mixed * mixed, axis=-1, keepdims=True) + eps_norm)
            result = mixed * inverse * gain[group : group + 1, :] * head_scale
            col = group * hv + h * vd
            mine[which, at, col : col + vd] = result.astype(jnp.bfloat16)

    for which in (1, 0):
        @pl.when(inner)
        def _():
            for group in range(2):
                def body(r, _, group=group):
                    attend(which, group, r)
                    return 0

                lax.fori_loop(0, nb, body, 0)
            if which == 1:
                lend(2).start()

        if which == 1:
            take(pick(0, 0, 1))
            to_mate([2], outer)
    take(pick(1, 1, last, False))

    @pl.when(outer)
    def _():
        lend(2).wait_recv()

    twin_start([others + 3])
    twin_wait([others + 3])
    tp_forward(head_gather, 0)
    tp_arrive(out_gather, tp_order[1:])
    take(pick(1, 0, 1))
    take(pick(0, 1, last))
    forward(2, 0, least=1, most=last)
    tp_arrive(head_gather, tp_order[1:])
    heads_all[tp_me] = turned[...]

    tall = math.gcd(rows, 128)
    count = rows // tall

    def swap(r, arriving):
        there = 1 - side if arriving else side
        view = normed.at[there, tp_me, pl.ds(pl.multiple_of(r * tall, tall), tall)]
        return pltpu.make_async_remote_copy(
            src_ref=view, dst_ref=view, send_sem=swap_sem.at[0, r], recv_sem=swap_sem.at[1, r],
            device_id={"sp": mate}, device_id_type=MESH,
        )

    def project(r, _):
        @pl.when(r > 0)
        def _():
            swap(r - 1, False).start()

        at = pl.ds(pl.multiple_of(r * tall, tall), tall)
        acc = residual[at, :].astype(jnp.float32)
        for d in range(tp):
            acc = acc + jnp.dot(heads_all[d, at, :], out_all[d], preferred_element_type=jnp.float32)
        inverse = lax.rsqrt(jnp.mean(acc * acc, axis=-1, keepdims=True) + eps_norm)
        scaled = (acc * inverse * ngain[...]).astype(jnp.bfloat16)
        for d in range(tp):
            normed[side, d, at, :] = scaled[:, d * share : (d + 1) * share]

            @pl.when(d == tp_me)
            def _():
                summed[at, :] = acc[:, d * share : (d + 1) * share]

        return 0

    copies[5].wait()
    lax.fori_loop(0, count, project, 0)
    swap(count - 1, False).start()
    norm_gathers = [
        (
            lambda slot, r=r: normed.at[1 - side, slot, pl.ds(r * tall, tall)], None,
            norm_send.at[r], norm_recv.at[r],
        )
        for r in range(count)
    ]
    take(pick(1, 1, last))
    for r in range(count):
        swap(r, True).wait_recv()
        tp_forward(norm_gathers[r], 0)
    to_mate([2], inner)
    take(pick(2, 1, last, False))
    take(pick(0, last, last + 1))
    take(pick(1, last, last + 1))

    step_cols = share // depth

    def feed(where):
        gate = jnp.zeros((rows, half), jnp.float32)
        upward = jnp.zeros((rows, half), jnp.float32)
        for s in range(n):
            low = (s % step_cols) * depth
            x = normed[where, s // step_cols, :, low : low + depth]
            gate = gate + lax.dot_general(x, wg_all[s], NT, preferred_element_type=jnp.float32)
            upward = upward + lax.dot_general(x, wu_all[s], NT, preferred_element_type=jnp.float32)
        hidden[where] = (gate / (1.0 + jnp.exp(-gate)) * upward).astype(jnp.bfloat16)

    def feed_one(i, _):
        @pl.when(i == 1)
        def _():
            for r in range(count):
                tp_arrive(norm_gathers[r], tp_order[1:])
            take(pick(2, 0, 1))
            take(pick(2, 1, last))

        feed((side + i) % 2)
        return 0

    lax.fori_loop(0, 2, feed_one, 0)
    cols = wd_all.shape[2]
    ratio = share // cols
    east = tp_me // 2

    def hand(src, dst, group, index, **target):
        return pltpu.make_async_remote_copy(
            src_ref=src, dst_ref=dst, send_sem=red_send.at[group, index], recv_sem=red_recv.at[group, index],
            device_id=target, device_id_type=MESH,
        )

    def near(index):
        return hand(near_out.at[index], near_in.at[index], 0, index, tp=flip(tp_me, 1))

    def far(low, where):
        return hand(far_out.at[low, where], far_in.at[low, where], 1, 2 * low + (where == side), tp=flip(tp_me, 2))

    def across(index):
        return hand(mate_out.at[index], mate_in.at[index], 2, index, sp=mate)

    def product(where, slab):
        return jnp.dot(hidden[where], wd_all[slab], preferred_element_type=jnp.float32)

    late = flip_all(sp_me, n - 1)

    def ready(slab):
        @pl.when(slab == late)
        def _():
            for a, mask in events:
                arrive(a, mask)

    def give(to_east, low):
        slab = (2 * to_east + 1 - core) * ratio + low
        index = to_east * ratio + low
        ready(slab)

        def one(where, _):
            near_out[index, where] = product(where, slab).astype(jnp.bfloat16)
            return 0

        lax.fori_loop(0, 2, one, 0)
        near(index).start()

    def relay(low):
        slab = (2 * (1 - east) + core) * ratio + low
        index = (1 - east) * ratio + low
        ready(slab)
        near(index).wait_recv()

        def one(where, _):
            both = product(where, slab) + near_in[index, where].astype(jnp.float32)
            far_out[low, where] = both.astype(jnp.bfloat16)
            return 0

        lax.fori_loop(0, 2, one, 0)
        far(low, 1 - side).start()
        far(low, side).start()

    def keep(low):
        slab = tp_me * ratio + low
        index = east * ratio + low
        ready(slab)
        near(index).wait_recv()

        def one(where, _):
            channel[low, where] = product(where, slab) + near_in[index, where].astype(jnp.float32)
            return 0

        lax.fori_loop(0, 2, one, 0)

    take([e for e in events if e[1] != n - 1])

    def reduce_one(i, _):
        low = (late + 1 + i) % ratio
        give(1 - east, low)
        relay(low)
        give(east, low)
        keep(low)
        return 0

    lax.fori_loop(0, ratio, reduce_one, 0)
    events.clear()
    for i in range(ratio):
        low = (late + 1 + i) % ratio
        far(low, 1 - side).wait_recv()
        both = channel[low, 1 - side] + far_in[low, 1 - side].astype(jnp.float32)
        mate_out[low] = both.astype(jnp.bfloat16)
        across(low).start()
        far(low, side).wait_recv()
        channel[low, side] = channel[low, side] + far_in[low, side].astype(jnp.float32)
    for low in range(ratio):
        across(low).wait_recv()
        final = channel[low, side] + mate_in[low].astype(jnp.float32)
        at = slice(low * cols, (low + 1) * cols)
        out[:, at] = (summed[:, at] + 0.5 * final).astype(jnp.bfloat16)

    for low in range(ratio):
        across(low).wait_send()
        for where in range(2):
            far(low, where).wait_send()
    for index in range(n // 2):
        near(index).wait_send()
    for r in range(count):
        swap(r, False).wait_send()
    for gather in [out_gather, head_gather] + norm_gathers:
        tp_drain(gather)
    for a in range(3):
        for mask in order[1:]:
            held, k = came[mask]
            cube(a, held, k, False).wait_send()

    @pl.when(apart)
    def _():
        for i in range(len(swaps)):
            twin(i).wait_send()

    @pl.when(outer)
    def _():
        lend(0).wait_send()
        lend(1).wait_send()

    @pl.when(inner)
    def _():
        lend(2).wait_send()
        for c in range(CHUNKS):
            for at in range(length):
                cross(c, at).wait_send()

    for c in range(CHUNKS):
        for at in range(length):
            for d in range(2):
                @pl.when(jnp.logical_and(rest[d], at <= line if d == 0 else at >= line))
                def _():
                    chain(c, d, at).wait_send()


def local(
    n, tp, residual, queries_a, keys_a, values_a, queries_b, keys_b, values_b, mix_lambda, head_gain,
    out_a, out_b, norm_gain, w_gate, w_up, w_down,
):
    rows, width = residual.shape
    share = width // tp
    units = w_gate.shape[1]
    hv = out_a.shape[0]
    cols = w_down.shape[1]
    tall = math.gcd(rows, 128)
    span = keys_a.shape[1] + keys_b.shape[1] + values_a.shape[1] + values_b.shape[1]
    vmem, anywhere = pl.BlockSpec(memory_space=pltpu.VMEM), pl.BlockSpec(memory_space=pl.ANY)
    smem = pl.BlockSpec(memory_space=pltpu.SMEM)
    bf16, f32 = jnp.bfloat16, jnp.float32
    dma = pltpu.SemaphoreType.DMA
    return pl.pallas_call(
        functools.partial(kernel, n, tp),
        out_shape=jax.ShapeDtypeStruct((rows, share), bf16),
        in_specs=[
            anywhere, anywhere, anywhere, anywhere, anywhere, anywhere, anywhere, smem, vmem,
            anywhere, anywhere, vmem, anywhere, anywhere, anywhere,
        ],
        out_specs=vmem,
        scratch_shapes=[
            pltpu.VMEM((n, rows, span), bf16),
            pltpu.VMEM((units, w_gate.shape[0]), bf16),
            pltpu.VMEM((units, w_gate.shape[0]), bf16),
            pltpu.VMEM((n, units // 2, w_gate.shape[0]), bf16),
            pltpu.VMEM((n, units // 2, w_gate.shape[0]), bf16),
            pltpu.VMEM((n, units // 2, w_down.shape[1]), bf16),
            pltpu.VMEM((tp, 2 * hv, width), bf16),
            pltpu.VMEM((tp, rows, 2 * hv), bf16),
            pltpu.VMEM((rows, share), f32),
            pltpu.VMEM((2, tp, rows, share), bf16),
            pltpu.VMEM((2, rows, units // 2), bf16),
            pltpu.VMEM((n // tp, 2, rows, cols), f32),
            pltpu.VMEM((n // 2, 2, rows, cols), bf16),
            pltpu.VMEM((n // 2, 2, rows, cols), bf16),
            pltpu.VMEM((n // tp, 2, rows, cols), bf16),
            pltpu.VMEM((n // tp, 2, rows, cols), bf16),
            pltpu.VMEM((n // tp, rows, cols), bf16),
            pltpu.VMEM((n // tp, rows, cols), bf16),
            pltpu.VMEM((2, rows, 2 * hv), bf16),
            pltpu.VMEM((rows, 2 * hv), bf16),
            pltpu.VMEM(residual.shape, bf16),
            pltpu.VMEM(w_gate.shape, bf16),
            pltpu.VMEM(w_up.shape, bf16),
            pltpu.VMEM((2,) + queries_a.shape, bf16),
            pltpu.VMEM((2,) + queries_b.shape, bf16),
            pltpu.VMEM((8 * -(-mix_lambda.size // 8), hv), f32),
            pltpu.VMEM((8 * -(-mix_lambda.size // 8), hv), f32),
            dma((3,)),
            dma((3,)),
            dma((6,)),
            dma((4 * CHUNKS + 4,)),
            dma((4 * CHUNKS + 4,)),
            dma((CHUNKS, 3, n // 2)),
            dma((CHUNKS, n // 2)),
            dma((CHUNKS, n // 2)),
            dma((3, n)),
            dma((3, n)),
            dma((tp - 1,)),
            dma((tp - 1,)),
            dma((tp - 1,)),
            dma((tp - 1,)),
            dma((2, rows // tall)),
            dma((rows // tall, tp - 1)),
            dma((rows // tall, tp - 1)),
            dma((3, n // 2)),
            dma((3, n // 2)),
        ],
        compiler_params=pltpu.CompilerParams(
            collective_id=0, has_side_effects=True, vmem_limit_bytes=63 * 1024 * 1024
        ),
        name="layer",
    )(
        residual, queries_a, keys_a, values_a, queries_b, keys_b, values_b, mix_lambda, head_gain,
        out_a, out_b, norm_gain.reshape(1, -1), w_gate, w_up, w_down,
    )


def solution(mesh):
    in_specs = (
        P("sp", None),
        P("sp", "tp"),
        P("sp", "tp"),
        P("sp", "tp"),
        P("sp", "tp"),
        P("sp", "tp"),
        P("sp", "tp"),
        P(None, "tp"),
        P(),
        P("tp", None),
        P("tp", None),
        P(),
        P("sp", "tp"),
        P("sp", "tp"),
        P("tp", "sp"),
    )
    body = functools.partial(local, mesh.shape["sp"], mesh.shape["tp"])
    return jax.shard_map(body, mesh=mesh, in_specs=in_specs, out_specs=P("sp", "tp"), check_vma=False)
```
